32 devices in a mesh: ep: 16 (over z, y, core), tp: 2 (over x).
Axes of the slice: x: 2, y: 2, z: 4, core: 2. Of those that a mesh axis runs over, the one named last changes fastest.
Arguments:
- tokens: bfloat16 [256, 2048], P('ep'), may hold values from -6 to 6
- lengths: int32 [256], P('ep'), may hold values from 256 to 1023
- cache: bfloat16 [256, 1024, 512], P('ep', None, 'tp'), may hold values from -6 to 6
- attn_gain: float32 [2048], replicated, may hold values from 0.1 to 1.9
- query_weight: bfloat16 [2048, 1024], P(None, 'tp'), may hold values from -0.125 to 0.125
- key_weight: bfloat16 [2048, 256], P(None, 'tp'), may hold values from -0.125 to 0.125
- value_weight: bfloat16 [2048, 256], P(None, 'tp'), may hold values from -0.125 to 0.125
- stick_bias: float32 [16], P('tp'), may hold values from -7 to -1
- out_weight: bfloat16 [1024, 2048], P('tp'), may hold values from -0.1875 to 0.1875
- ffn_gain: float32 [2048], replicated, may hold values from 0.1 to 1.9
- routes: int32 [256, 6], P('ep'), may hold values from 0 to 15, all different within a row; in each aligned block of 16 rows (0 to 15, 16 to 31, ...) at most 12 rows name the same one
- route_weights: float32 [256, 6], P('ep'), may hold values from 0.1 to 0.6
- expert_gate: bfloat16 [16, 2048, 1024], P('ep', None, 'tp'), may hold values from -0.125 to 0.125
- expert_up: bfloat16 [16, 2048, 1024], P('ep', None, 'tp'), may hold values from -0.125 to 0.125
- expert_down: bfloat16 [16, 1024, 2048], P('ep', 'tp'), may hold values from -0.1875 to 0.1875
- shared_gate: bfloat16 [2048, 512], P('ep', 'tp'), may hold values from -0.125 to 0.125
- shared_up: bfloat16 [2048, 512], P('ep', 'tp'), may hold values from -0.125 to 0.125
- shared_down: bfloat16 [512, 2048], P('tp'), may hold values from -0.25 to 0.25
- gate_vector: bfloat16 [2048], replicated, may hold values from -0.125 to 0.125
Outputs:
- layer_out: bfloat16 [256, 2048], P('ep', 'tp')
- new_kv: bfloat16 [256, 512], P('ep', 'tp')
The draws below stay inside these ranges and needn't reach their ends.
Inputs may be any that keep to these rules, and one draw needn't show every extreme that they name: Each sequence's new token comes after its lengths cached positions. `routes`: each row names 6 different experts; among the 16 rows of one index of ep no expert is named by more than 12 rows.
All inputs are finite; a program needn't handle non-finite values.
Results may differ from the reference program's by a relative error of at most 0.012.
Values may be sent and summed in bfloat16 or wider, within the bound.
A program may use at most 64 MiB of HBM per device.

```python
import math
import jax
import jax.numpy as jnp
import numpy as np
from jax import lax

D = 2048
HEAD_DIM = 64
Q_HEADS = 16
KV_HEADS = 4
EXPERT_FF = 1024
SHARED_FF = 512
TOP_K = 6
SEQ_DEV = 16
CACHE = 1024
SEQS = 256
EXPERTS = 16
CAP = 12
N_EP = 16
N_TP = 2


def touch_ends(entries, own_key, low, largest):
    shape = entries.shape
    index_at = [jax.random.randint(jax.random.fold_in(own_key, axis), (), 0, shape[axis]) for axis in range(len(shape))]
    entries = entries.at[tuple(index_at)].set(low)
    longest = shape.index(max(shape))
    index_at[longest] = (index_at[longest] + 1) % shape[longest]
    return entries.at[tuple(index_at)].set(largest)


def steps_of(stream_key, dims, cuts, low, largest):
    def one(axis_at, parts):
        steps = jax.random.uniform(jax.random.fold_in(jax.random.fold_in(stream_key, 6), axis_at), (parts,), jnp.float32, low / len(cuts), largest / len(cuts))
        return jnp.repeat(jnp.exp(steps), dims[axis_at] // parts).reshape((-1,) + (1,) * (len(dims) - axis_at - 1))

    factor_of = one(*cuts[0])
    for cut in cuts[1:]:
        factor_of = factor_of * one(*cut)
    return factor_of


def routed_block(rng, own, number, rows, count, top, bound, lean):
    sequence = jax.random.permutation(rng, count)
    heavy_load, usual = shares(count, rows * top, bound, lean, True), shares(count, rows * top, bound, lean, False)
    places = jnp.arange(count)

    def named(tallies, turn):
        used = int((tallies > 0).sum())
        fixed = max(1, used // 4)
        passed = fixed + (places - fixed + turn * (used - fixed)) % max(1, count - fixed)
        return jnp.zeros((count,), jnp.int32).at[sequence[jnp.where(places < fixed, places, passed)]].set(jnp.asarray(tallies, jnp.int32))

    tallies = jnp.where(number % 4 == 0, named(heavy_load, number // 4), named(usual, number - number // 4 - 1))
    mixed = jax.random.permutation(jax.random.fold_in(own, 3), count)
    source_of, sink = mixed[0:count // 2 * 2:2], mixed[1:count // 2 * 2:2]
    slack = jnp.minimum(tallies[source_of] - 1, bound - tallies[sink]) // 2
    slack = jnp.where((source_of == sequence[0]) | (sink == sequence[0]) | (tallies[sink] == 0), 0, jnp.maximum(slack, 0))
    passed = jax.random.randint(jax.random.fold_in(own, 4), (count // 2,), 0, 1 << 20) % (slack + 1)
    tallies = tallies.at[source_of].add(-passed).at[sink].add(passed)
    items = jnp.searchsorted(jnp.cumsum(tallies), jnp.arange(rows * top), side="right").astype(jnp.int32)
    table = items.reshape(top, rows).T
    table = table[jax.random.permutation(jax.random.fold_in(own, 1), rows)]
    turn = jax.random.randint(jax.random.fold_in(own, 2), (rows, 1), 0, top)
    return jnp.take_along_axis(table, (jnp.arange(top)[None, :] + turn) % top, axis=1)


def shares(count, total, most, skew, full):
    loads = [(1 << 20) // math.isqrt(standing ** skew) + 1 for standing in range(1, count + 1)]
    largest = most if full else min(most, max(-(-total // count), total * loads[0] // sum(loads)))
    least = 1 if total - largest >= count - 1 else 0
    given, surplus = [largest] + [least] * (count - 1), total - largest - least * (count - 1)
    while surplus > 0:
        free = [i for i in range(1, count) if given[i] < largest] or [i for i in range(1, count) if given[i] < most]
        pool, remaining = sum([loads[i] for i in free]), surplus
        for i in free:
            addition = min(most - given[i], max(1, remaining * loads[i] // pool), surplus)
            given[i] = given[i] + addition
            surplus = surplus - addition
    return np.array(given)


def noise(rng, shape, spread, most, shards=(), kind=jnp.bfloat16):
    values = jax.random.normal(rng, shape, jnp.float32) * spread
    if len(shards) > 0:
        values = steps_of(rng, shape, shards, -0.22, 0.18) * values
    return jnp.clip(values, min=-most, max=most).astype(kind)


def setup_inputs(seed: int = 0) -> dict:
    splits = jax.random.split(jax.random.key(seed), 20)
    tokens = noise(splits[0], (SEQS, D), 1.0, 6.0, ((0, 16),))
    lengths = touch_ends(jax.random.randint(splits[1], (SEQS,), CACHE // 4, CACHE), jax.random.fold_in(splits[1], 1), CACHE // 4, CACHE - 1).astype(jnp.int32)
    cache = noise(splits[2], (SEQS, CACHE, 2 * KV_HEADS * HEAD_DIM), 1.0, 6.0, ((0, 16), (2, 2)))
    attn_gain = jnp.clip(1.0 + 0.18 * jax.random.normal(splits[3], (D,), jnp.float32), 0.1, 1.9)
    query_weight = noise(splits[4], (D, Q_HEADS * HEAD_DIM), D ** -0.5, 0.125, ((1, 2),))
    key_weight = noise(splits[5], (D, KV_HEADS * HEAD_DIM), D ** -0.5, 0.125, ((1, 2),))
    value_weight = noise(splits[6], (D, KV_HEADS * HEAD_DIM), D ** -0.5, 0.125, ((1, 2),))
    stick_bias = jnp.clip(-7.0 + 6.0 * jax.random.uniform(splits[7], (Q_HEADS,), jnp.float32) ** steps_of(splits[7], (Q_HEADS,), ((0, 2),), -0.2, 0.2), -7.0, -1.0)
    out_weight = noise(splits[8], (Q_HEADS * HEAD_DIM, D), (Q_HEADS * HEAD_DIM) ** -0.5, 0.1875, ((0, 2),))
    ffn_gain = jnp.clip(1.0 + 0.18 * jax.random.normal(splits[9], (D,), jnp.float32), 0.1, 1.9)
    routes_keys = jax.random.split(jax.random.fold_in(splits[10], 1), SEQS // SEQ_DEV)
    routes_turns = jax.random.permutation(jax.random.fold_in(splits[10], 3), SEQS // SEQ_DEV)
    routes = jax.vmap(lambda own, number: routed_block(jax.random.fold_in(splits[10], 2), own, number, SEQ_DEV, EXPERTS, TOP_K, CAP, 1))(routes_keys, routes_turns).reshape((SEQS, TOP_K))
    route_weights = jnp.clip(0.1 + 0.5 * jax.random.uniform(splits[11], (SEQS, TOP_K), jnp.float32) ** steps_of(splits[11], (SEQS, TOP_K), ((0, 16),), -0.2, 0.2), 0.1, 0.6)
    expert_gate = noise(splits[12], (EXPERTS, D, EXPERT_FF), D ** -0.5, 0.125, ((0, 16), (2, 2)))
    expert_up = noise(splits[13], (EXPERTS, D, EXPERT_FF), D ** -0.5, 0.125, ((0, 16), (2, 2)))
    expert_down = noise(splits[14], (EXPERTS, EXPERT_FF, D), EXPERT_FF ** -0.5, 0.1875, ((0, 16), (1, 2)))
    shared_gate = noise(splits[15], (D, SHARED_FF), D ** -0.5, 0.125, ((0, 16), (1, 2)))
    shared_up = noise(splits[16], (D, SHARED_FF), D ** -0.5, 0.125, ((0, 16), (1, 2)))
    shared_down = noise(splits[17], (SHARED_FF, D), SHARED_FF ** -0.5, 0.25, ((0, 2),))
    gate_vector = noise(splits[18], (D,), D ** -0.5, 0.125)
    return dict(tokens=tokens, lengths=lengths, cache=cache, attn_gain=attn_gain, query_weight=query_weight, key_weight=key_weight, value_weight=value_weight, stick_bias=stick_bias, out_weight=out_weight, ffn_gain=ffn_gain, routes=routes, route_weights=route_weights, expert_gate=expert_gate, expert_up=expert_up, expert_down=expert_down, shared_gate=shared_gate, shared_up=shared_up, shared_down=shared_down, gate_vector=gate_vector)


epsilon = 1e-06

def rms_scale(rows_in, gain_row):
    values_f = rows_in.astype(jnp.float32)
    return values_f * lax.rsqrt(lax.optimization_barrier(jnp.mean(values_f * values_f, axis=-1, keepdims=True)) + epsilon) * gain_row

def block_sum(left_rows, right_rows, blocks):
    row_count, inner = left_rows.shape
    part_width = inner // blocks
    left_view = left_rows.reshape(row_count, blocks, part_width).astype(jnp.float32)
    right_view = right_rows.reshape(blocks, part_width, right_rows.shape[1]).astype(jnp.float32)
    partials = jnp.einsum('nbf,bfd->bnd', left_view, right_view).astype(jnp.bfloat16)
    return lax.optimization_barrier(jnp.sum(partials.astype(jnp.float32), axis=0))

def reference(tokens, lengths, cache, attn_gain, query_weight, key_weight, value_weight, stick_bias, out_weight, ffn_gain, routes, route_weights, expert_gate, expert_up, expert_down, shared_gate, shared_up, shared_down, gate_vector):
    total_rows = tokens.shape[0]
    normed = rms_scale(tokens, attn_gain).astype(jnp.bfloat16)
    queries = jnp.dot(normed, query_weight, preferred_element_type=jnp.float32).astype(jnp.bfloat16)
    key_rows = jnp.dot(normed, key_weight, preferred_element_type=jnp.float32).astype(jnp.bfloat16)
    value_rows = jnp.dot(normed, value_weight, preferred_element_type=jnp.float32).astype(jnp.bfloat16)
    new_kv = jnp.stack([key_rows.reshape(total_rows, KV_HEADS, HEAD_DIM), value_rows.reshape(total_rows, KV_HEADS, HEAD_DIM)], axis=2)
    new_kv = new_kv.reshape(total_rows, 2 * KV_HEADS * HEAD_DIM)
    group_size = Q_HEADS // KV_HEADS
    grouped = queries.reshape(N_EP, SEQ_DEV, KV_HEADS, group_size, HEAD_DIM)
    cache_view = cache.reshape(N_EP, SEQ_DEV, CACHE, KV_HEADS, 2, HEAD_DIM)
    span_rows = lengths.reshape(N_EP, SEQ_DEV)
    offsets = stick_bias.astype(jnp.float32).reshape(1, KV_HEADS, group_size, 1)

    def attend(pieces):
        query_block, cache_block, span_block = pieces
        key_block = cache_block[:, :, :, 0, :].astype(jnp.float32)
        value_block = cache_block[:, :, :, 1, :].astype(jnp.float32)
        scores = jnp.einsum('nkgd,nckd->nkgc', query_block.astype(jnp.float32), key_block) * HEAD_DIM ** (-0.5)
        scores = scores + offsets
        positions = jnp.arange(CACHE, dtype=jnp.int32)
        usable = (positions[None, :] < span_block[:, None])[:, None, None, :]
        log_keep = jnp.where(usable, jax.nn.log_sigmoid(-scores), 0.0)
        behind = lax.cumsum(log_keep, axis=3, reverse=True) - log_keep
        stick_weights = jnp.where(usable, jnp.exp(jax.nn.log_sigmoid(scores) + behind), 0.0).astype(jnp.bfloat16)
        mixed = jnp.einsum('nkgc,nckd->nkgd', stick_weights.astype(jnp.float32), value_block)
        return mixed.astype(jnp.bfloat16)
    heads_out = lax.map(attend, (grouped, cache_view, span_rows)).reshape(total_rows, Q_HEADS * HEAD_DIM)
    residual = tokens.astype(jnp.float32) + block_sum(heads_out, out_weight, N_TP)
    normed_mix = rms_scale(residual, ffn_gain).astype(jnp.bfloat16)
    flat_routes = routes.reshape(-1)
    flat_weights = route_weights.reshape(-1).astype(jnp.float32)
    rows_most = N_EP * CAP

    def run_expert(expert_index):
        routed_here = flat_routes == expert_index
        ordering = jnp.argsort(jnp.where(routed_here, 0, 1).astype(jnp.int32), stable=True)[:rows_most]
        ordering = ordering.astype(jnp.int32)
        owners = (ordering // TOP_K).astype(jnp.int32)
        chosen = normed_mix[owners]
        gate_val = jnp.dot(chosen, expert_gate[expert_index], preferred_element_type=jnp.float32)
        up_val = jnp.dot(chosen, expert_up[expert_index], preferred_element_type=jnp.float32)
        hidden = (jax.nn.silu(gate_val) * up_val).astype(jnp.bfloat16)
        result = block_sum(hidden, expert_down[expert_index], N_TP).astype(jnp.bfloat16)
        route_scale = jnp.where(routed_here[ordering], flat_weights[ordering], 0.0)
        return (owners, result.astype(jnp.float32) * route_scale[:, None])
    owner_rows, contrib = lax.map(run_expert, jnp.arange(EXPERTS, dtype=jnp.int32))
    routed = jnp.zeros((total_rows, D), jnp.float32).at[owner_rows.reshape(-1)].add(contrib.reshape(-1, D))
    shared_gate_val = jnp.dot(normed_mix, shared_gate, preferred_element_type=jnp.float32)
    shared_up_val = jnp.dot(normed_mix, shared_up, preferred_element_type=jnp.float32)
    shared_hidden = (jax.nn.silu(shared_gate_val) * shared_up_val).astype(jnp.bfloat16)
    shared_out = block_sum(shared_hidden, shared_down, N_TP)
    mix_gate = jax.nn.sigmoid(jnp.dot(normed_mix, gate_vector, preferred_element_type=jnp.float32))
    layer_out = (residual + routed + mix_gate[:, None] * shared_out).astype(jnp.bfloat16)
    return (layer_out, new_kv)
```

```python
import functools

import jax
import jax.numpy as jnp
from jax import lax
from jax.experimental import pallas as pl
from jax.experimental.pallas import tpu as pltpu
from jax.sharding import PartitionSpec as P

HEAD_DIM = 64
LANES = 128
GROUPS = 2
CHUNKS = 2
epsilon = 1e-06
MESH = pl.DeviceIdType.MESH
F32 = jnp.float32
BF16 = jnp.bfloat16


def normalise(values, gain):
    return (
        values * lax.rsqrt(jnp.mean(values * values, axis=-1, keepdims=True) + epsilon) * gain
    ).astype(BF16)


def layer_kernel(
    ranks_ep,
    ranks_tp,
    tokens_hbm,
    lengths_hbm,
    cache_hbm,
    attn_gain_hbm,
    query_hbm,
    key_hbm,
    value_hbm,
    bias_hbm,
    out_hbm,
    ffn_gain_hbm,
    routes_hbm,
    portions_hbm,
    gate_hbm,
    up_hbm,
    down_hbm,
    sgate_hbm,
    sup_hbm,
    sdown_hbm,
    vector_hbm,
    out_ref,
    kv_ref,
    tokens_ref,
    span_ref,
    held,
    attn_gain_ref,
    query_w,
    key_w,
    value_w,
    bias_ref,
    out_w,
    ffn_gain_ref,
    routes_ref,
    portions_ref,
    gate_w,
    up_w,
    down_w,
    sgate_w,
    sup_w,
    sdown_w,
    vector_ref,
    normed_ref,
    logits,
    spread,
    partial,
    attn_in,
    residual_ref,
    gathered,
    hidden_ref,
    terms,
    core_in,
    mid,
    x_in,
    fin,
    fin_in,
    sh_own,
    sh_in,
    sh_mid,
    sh_fin,
    sh_out,
    sh_x,
    load_sem,
    cache_sem,
    swap_send,
    swap_recv,
    ag_send,
    ag_recv,
    core_send,
    core_recv,
    x_send,
    x_recv,
    fin_send,
    fin_recv,
    shc_send,
    shc_recv,
    shf_send,
    shf_recv,
    shx_send,
    shx_recv,
):
    me = lax.axis_index("ep")
    my_tp = lax.axis_index("tp")
    row_count, width = tokens_ref.shape
    groups = gathered.shape[0]
    rows = row_count // groups
    experts = gate_w.shape[0]
    table_width = gathered.shape[2] - width
    all_rows = ranks_ep * rows
    half = ranks_ep // 2
    half_rows = half * rows
    heads = spread.shape[1]
    tiles = spread.shape[2] // LANES
    group = heads // tiles
    quarter = width // ranks_tp
    chunks = terms.shape[1]
    chunk_width = quarter // chunks
    chips = ranks_ep // 2
    across = 1 << (chips.bit_length() - 1) // 2
    zmasks = [m * 2 * across for m in range(chips // across - 1, 0, -1)]
    ymasks = [m * 2 for m in range(across - 1, 0, -1)]
    away = [z + y for z in (*zmasks, 0) for y in (*ymasks, 0) if z + y]

    def flip(mask):
        index = me
        weight = 1
        while weight <= mask:
            if mask & weight:
                index = index + (1 - 2 * ((me // weight) % 2)) * weight
            weight = weight * 2
        return index

    def peer(step):
        return lax.rem(my_tp + step, ranks_tp)

    loads = {}

    def load(name, source, target):
        copy = pltpu.make_async_copy(source, target, load_sem.at[len(loads)])
        copy.start()
        loads[name] = copy

    caches = []

    def load_caches(g):
        for s in range(g * rows, (g + 1) * rows):
            copy = pltpu.make_async_copy(cache_hbm.at[s], held.at[s], cache_sem.at[s])
            copy.start()
            caches.append(copy)

    load("tokens", tokens_hbm, tokens_ref)
    load("attn_gain", attn_gain_hbm, attn_gain_ref)
    load("query", query_hbm, query_w)
    load("lengths", lengths_hbm, span_ref)
    load("bias", bias_hbm, bias_ref)
    load_caches(0)
    barrier = pltpu.get_barrier_semaphore()
    for mask in (*away, 1):
        pl.semaphore_signal(barrier, inc=1, device_id={"ep": flip(mask)}, device_id_type=MESH)
    for step in range(1, ranks_tp):
        pl.semaphore_signal(barrier, inc=1, device_id={"tp": peer(step)}, device_id_type=MESH)

    loads["tokens"].wait()
    loads["attn_gain"].wait()
    normed_ref[...] = normalise(tokens_ref[...].astype(F32), attn_gain_ref[...])
    loads["query"].wait()
    load("out", out_hbm, out_w)
    for g in range(1, groups):
        load_caches(g)
    load("ffn_gain", ffn_gain_hbm, ffn_gain_ref)
    load("routes", routes_hbm, routes_ref)
    load("portions", portions_hbm, portions_ref)
    load("vector", vector_hbm, vector_ref)
    queries = jnp.dot(normed_ref[...], query_w[...], preferred_element_type=F32).astype(BF16).astype(F32)
    queries = queries * HEAD_DIM ** (-0.5)
    spread[...] = jnp.zeros_like(spread)
    first_half = lax.broadcasted_iota(jnp.int32, (row_count, LANES), 1) < HEAD_DIM
    for h in range(heads):
        pair = queries[:, h // 2 * LANES : (h // 2 + 1) * LANES]
        if h % 2:
            pair = pltpu.roll(pair, HEAD_DIM, 1)
        tile = h // group * LANES
        spread[:, h, tile : tile + LANES] = jnp.where(first_half, pair, 0.0)
    loads["lengths"].wait()
    loads["bias"].wait()

    length = held.shape[1]
    block = 256
    count = length // block
    lines = rows * heads

    def attend(g):
        first = g * rows
        for s in range(first, first + rows):
            caches[s].wait()
        for s in range(first, first + rows):
            logits[(s - first) * heads : (s - first + 1) * heads, :] = lax.dot_general(
                spread[s].astype(BF16), held[s], (((1,), (1,)), ((), ())), preferred_element_type=F32
            )
        row = lax.broadcasted_iota(jnp.int32, (lines, 1), 0)
        limit = jnp.zeros((lines, 1), jnp.int32)
        for s in range(rows):
            limit = jnp.where(row // heads == s, span_ref[first + s], limit)
        offset = jnp.zeros((lines, 1), F32)
        for h in range(heads):
            offset = jnp.where(row % heads == h, bias_ref[h], offset)
        table = (
            lax.broadcasted_iota(jnp.int32, (block, block), 0)
            >= lax.broadcasted_iota(jnp.int32, (block, block), 1)
        ).astype(F32).astype(BF16)
        position = lax.broadcasted_iota(jnp.int32, (lines, block), 1)
        parts = []
        for b in range(count):
            cols = slice(b * block, (b + 1) * block)
            z = logits[:, cols] + offset
            usable = position + b * block < limit
            soft = jnp.where(usable, jnp.maximum(z, 0.0) + jnp.log(1.0 + jnp.exp(-jnp.abs(z))), 0.0)
            logits[:, cols] = jnp.where(usable, z, -1e30)
            high = soft.astype(BF16)
            parts.append((high, (soft - high.astype(F32)).astype(BF16)))
        sums = [
            jnp.dot(high, table, preferred_element_type=F32)
            + jnp.dot(low, table, preferred_element_type=F32)
            for high, low in parts
        ]
        carried = jnp.zeros((lines, 1), F32)
        for b in range(count - 1, -1, -1):
            cols = slice(b * block, (b + 1) * block)
            logits[:, cols] = jnp.exp(logits[:, cols] - sums[b] - carried)
            carried = carried + sums[b][:, :1]
        for s in range(first, first + rows):
            spread[s] = jnp.dot(
                logits[(s - first) * heads : (s - first + 1) * heads, :].astype(BF16),
                held[s],
                preferred_element_type=F32,
            )
        upper = lax.broadcasted_iota(jnp.int32, (rows, LANES), 1) < HEAD_DIM
        gathered_heads = []
        for i in range(heads // 2):
            pair = []
            for h in (2 * i, 2 * i + 1):
                tile = h // group * LANES
                pair.append(spread[first : first + rows, h, tile : tile + LANES])
            gathered_heads.append(jnp.where(upper, pltpu.roll(pair[0], HEAD_DIM, 1), pair[1]))
        return jnp.concatenate(gathered_heads, axis=1).astype(BF16)

    swaps = {}

    def swap(g, heads_out):
        partial[g] = jnp.dot(heads_out, out_w[...], preferred_element_type=F32).astype(BF16)
        for step in range(1, ranks_tp):
            copy = pltpu.make_async_remote_copy(
                src_ref=partial.at[g],
                dst_ref=attn_in.at[g, step - 1],
                send_sem=swap_send.at[g, step - 1],
                recv_sem=swap_recv.at[g, step - 1],
                device_id={"tp": peer(step)},
                device_id_type=MESH,
            )
            copy.start()
            swaps[g, step] = copy

    def spot(mask):
        return (mask % 2 * half + mask // 2) * rows

    sent = []
    arrivals = {}
    shares = [0] * groups

    def share(g, source, goal):
        slot = source ^ goal
        copy = pltpu.make_async_remote_copy(
            src_ref=gathered.at[g, pl.ds(spot(source), rows)],
            dst_ref=gathered.at[g, pl.ds(spot(slot), rows)],
            send_sem=ag_send.at[g, shares[g]],
            recv_sem=ag_recv.at[g, slot],
            device_id={"ep": flip(goal)},
            device_id_type=MESH,
        )
        copy.start()
        shares[g] += 1
        sent.append(copy)
        arrivals[g, slot] = copy

    def spread_tokens(g):
        own = slice(g * rows, (g + 1) * rows)
        residual = partial[g].astype(F32)
        for step in range(1, ranks_tp):
            swaps[g, step].wait_recv()
            residual = residual + attn_in[g, step - 1].astype(F32)
        residual = residual + tokens_ref[own, :].astype(F32)
        residual_ref[own, :] = residual
        normed = normalise(residual, ffn_gain_ref[...])
        gathered[g, 0:rows, :width] = normed
        for mask in (*zmasks, *ymasks, 1):
            share(g, 0, mask)
        return jax.nn.sigmoid(
            jnp.sum(
                normed.astype(F32) * vector_ref[...].astype(F32).reshape(1, width), axis=1, keepdims=True
            )
        )

    def pass_near(g):
        for z in zmasks:
            arrivals[g, z].wait_recv()
            for y in ymasks:
                share(g, z, y)
            share(g, z, 1)
        for y in ymasks:
            arrivals[g, y].wait_recv()
            share(g, y, 1)

    def pass_far(g):
        for z in zmasks:
            for y in ymasks:
                arrivals[g, z + y].wait_recv()
                share(g, z + y, 1)

    def collect(g):
        for mask in (*away, 0):
            arrivals[g, mask + 1].wait_recv()

    shared_cols = sgate_w.shape[1]
    depth = sgate_w.shape[0]

    def push(source, target, send_sem, recv_sem, device):
        copy = pltpu.make_async_remote_copy(
            src_ref=source,
            dst_ref=target,
            send_sem=send_sem,
            recv_sem=recv_sem,
            device_id=device,
            device_id_type=MESH,
        )
        copy.start()
        sent.append(copy)
        return copy

    moves = {}

    def shared_in(g):
        feature_at = pl.ds(pl.multiple_of(me * (width // ranks_ep) // depth * depth, depth), depth)
        features = gathered[g, :, feature_at]
        for i, part in enumerate((sgate_w, sup_w)):
            sh_own[g, :, i * shared_cols : (i + 1) * shared_cols] = jnp.dot(
                features, part[...], preferred_element_type=F32
            ).astype(BF16)
        moves["shc", g] = push(
            sh_own.at[g, pl.ds(half_rows, half_rows)],
            sh_in.at[g],
            shc_send.at[g],
            shc_recv.at[g],
            {"ep": flip(1)},
        )

    def expert_in(g):
        inputs = gathered[g, :, :width]
        route_cols = gathered[g, :, width:].astype(F32)
        lanes = lax.broadcasted_iota(jnp.int32, route_cols.shape, 1)
        stride = table_width // 2
        scales = []
        for j in range(experts):
            wanted = me * experts + j
            chosen = jnp.where((lanes == wanted) | (lanes == wanted + stride), route_cols, 0.0)
            scales.append(jnp.sum(chosen, axis=1, keepdims=True))
            gate_val = jnp.dot(inputs, gate_w[j], preferred_element_type=F32)
            up_val = jnp.dot(inputs, up_w[j], preferred_element_type=F32)
            hidden_ref[g, j] = (gate_val * jax.nn.sigmoid(gate_val) * up_val).astype(BF16)
        return scales

    def expert_out(g, scales):
        for c in range(chunks):
            for step in range(ranks_tp):
                start = peer(step) * quarter + c * chunk_width
                cols = pl.ds(pl.multiple_of(start, chunk_width), chunk_width)
                term = jnp.zeros((all_rows, chunk_width), F32)
                for j in range(experts):
                    term = term + scales[j] * jnp.dot(
                        hidden_ref[g, j], down_w[j, :, cols], preferred_element_type=F32
                    )
                terms[g, c, step] = term.astype(BF16)
            moves["core", g, c] = push(
                terms.at[g, c, :, pl.ds(half_rows, half_rows)],
                core_in.at[g, c],
                core_send.at[g, c],
                core_recv.at[g, c],
                {"ep": flip(1)},
            )

    def shared_far(g):
        moves["shc", g].wait_recv()
        sh_mid[g] = (sh_own[g, :half_rows].astype(F32) + sh_in[g].astype(F32)).astype(BF16)
        for i, mask in enumerate(away):
            moves["shf", g, i] = push(
                sh_mid.at[g, pl.ds(spot(mask), rows)],
                sh_fin.at[g, i],
                shf_send.at[g, i],
                shf_recv.at[g, i],
                {"ep": flip(mask)},
            )

    def cross(g):
        for c in range(chunks):
            moves["core", g, c].wait_recv()
            for step in (*range(1, ranks_tp), 0):
                mid[g, c, step] = (
                    terms[g, c, step, :half_rows].astype(F32) + core_in[g, c, step].astype(F32)
                ).astype(BF16)
                if step:
                    moves["x", g, c, step] = push(
                        mid.at[g, c, step],
                        x_in.at[g, c, step - 1],
                        x_send.at[g, c, step - 1],
                        x_recv.at[g, c, step - 1],
                        {"tp": peer(step)},
                    )

    def deliver(g):
        for c in range(chunks):
            total = mid[g, c, 0].astype(F32)
            for step in range(1, ranks_tp):
                moves["x", g, c, step].wait_recv()
                total = total + x_in[g, c, step - 1].astype(F32)
            fin[g, c] = total.astype(BF16)
            for i, mask in enumerate(away):
                moves["fin", g, c, i] = push(
                    fin.at[g, c, pl.ds(spot(mask), rows)],
                    fin_in.at[g, c, i],
                    fin_send.at[g, c, i],
                    fin_recv.at[g, c, i],
                    {"ep": flip(mask)},
                )

    def quarter_of(index):
        return pl.ds(pl.multiple_of(index * quarter, quarter), quarter)

    def shared_end(g):
        total = sh_mid[g, 0:rows].astype(F32)
        for i in range(len(away)):
            moves["shf", g, i].wait_recv()
            total = total + sh_fin[g, i].astype(F32)
        gate_sum = total[:, :shared_cols]
        up_sum = total[:, shared_cols:]
        hidden = (gate_sum * jax.nn.sigmoid(gate_sum) * up_sum).astype(BF16)
        for step in range(1, ranks_tp):
            sh_out[g, step] = jnp.dot(
                hidden, sdown_w[:, quarter_of(peer(step))], preferred_element_type=F32
            ).astype(BF16)
            moves["shx", g, step] = push(
                sh_out.at[g, step],
                sh_x.at[g, step - 1],
                shx_send.at[g, step - 1],
                shx_recv.at[g, step - 1],
                {"tp": peer(step)},
            )
        sh_out[g, 0] = jnp.dot(
            hidden, sdown_w[:, quarter_of(my_tp)], preferred_element_type=F32
        ).astype(BF16)

    def finish(g, mix_gate):
        own = slice(g * rows, (g + 1) * rows)
        shared = sh_out[g, 0].astype(F32)
        for step in range(1, ranks_tp):
            moves["shx", g, step].wait_recv()
            shared = shared + sh_x[g, step - 1].astype(F32)
        base = residual_ref[own, quarter_of(my_tp)] + mix_gate * shared
        for c in range(chunks):
            cols = slice(c * chunk_width, (c + 1) * chunk_width)
            total = fin[g, c, 0:rows].astype(F32)
            for i in range(len(away)):
                moves["fin", g, c, i].wait_recv()
                total = total + fin_in[g, c, i].astype(F32)
            out_ref[own, cols] = (base[:, cols] + total).astype(out_ref.dtype)

    scope = jax.named_scope
    mix_gates = []
    scales = []
    for g in range(groups):
        with scope(f"attend{g}"):
            heads_out = attend(g)
        if g == 0:
            loads["out"].wait()
            load("key", key_hbm, key_w)
            load("value", value_hbm, value_w)
            load("sgate", sgate_hbm, sgate_w)
            load("sup", sup_hbm, sup_w)
            load("gate", gate_hbm, gate_w)
            load("up", up_hbm, up_w)
            load("down", down_hbm, down_w)
            load("sdown", sdown_hbm, sdown_w)
            with scope("barrier"):
                pl.semaphore_wait(barrier, len(away) + ranks_tp)
        with scope(f"swap{g}"):
            swap(g, heads_out)

    lane = lax.broadcasted_iota(jnp.int32, (row_count, table_width), 1)
    stride = table_width // 2
    table = jnp.zeros((row_count, table_width), F32)
    loads["routes"].wait()
    loads["portions"].wait()
    route_ids = jnp.transpose(routes_ref[...])
    portions = jnp.transpose(portions_ref[...])
    for k in range(routes_ref.shape[0]):
        named = route_ids[:, k : k + 1]
        portion = portions[:, k : k + 1]
        high = portion.astype(BF16).astype(F32)
        table = jnp.where(lane == named, high, table)
        table = jnp.where(lane == named + stride, portion - high, table)
    for g in range(groups):
        gathered[g, 0:rows, width:] = table[g * rows : (g + 1) * rows].astype(BF16)
    loads["ffn_gain"].wait()
    loads["vector"].wait()
    for g in range(groups):
        with scope(f"tokens{g}"):
            mix_gates.append(spread_tokens(g))
        if g == 0:
            with scope("kv"):
                loads["key"].wait()
                loads["value"].wait()
                key_rows = jnp.dot(normed_ref[...], key_w[...], preferred_element_type=F32)
                value_rows = jnp.dot(normed_ref[...], value_w[...], preferred_element_type=F32)
                pieces = []
                for h in range(key_w.shape[1] // HEAD_DIM):
                    cols = slice(h * HEAD_DIM, (h + 1) * HEAD_DIM)
                    pieces += [key_rows[:, cols], value_rows[:, cols]]
                kv_ref[...] = jnp.concatenate(pieces, axis=1).astype(BF16)
    for name in ("sgate", "sup", "gate", "up", "down", "sdown"):
        loads[name].wait()
    for g in range(groups):
        with scope(f"near{g}"):
            pass_near(g)
    for g in range(groups):
        if g == 0:
            with scope(f"far{g}"):
                pass_far(g)
        with scope(f"collect{g}"):
            collect(g)
        with scope(f"shin{g}"):
            shared_in(g)
        with scope(f"expin{g}"):
            scales.append(expert_in(g))
        if g + 1 < groups:
            with scope(f"far{g+1}"):
                pass_far(g + 1)
        with scope(f"expout{g}"):
            expert_out(g, scales[g])
        with scope(f"shfar{g}"):
            shared_far(g)
        if g + 1 < groups:
            with scope(f"cross{g}"):
                cross(g)
    for g in range(groups - 1):
        with scope(f"deliver{g}"):
            deliver(g)
    with scope(f"cross{groups-1}"):
        cross(groups - 1)
    for g in range(groups):
        with scope(f"shend{g}"):
            shared_end(g)
    with scope(f"deliver{groups-1}"):
        deliver(groups - 1)
    for g in range(groups):
        with scope(f"finish{g}"):
            finish(g, mix_gates[g])
    with scope("sends"):
        for copy in swaps.values():
            copy.wait_send()
        for copy in sent:
            copy.wait_send()


def layer(ranks_ep, ranks_tp, *operands):
    tokens, lengths, cache, _, query, key, value, bias, out_weight = operands[:9]
    _, routes, portions, gate, up, down, sgate, sup, sdown, vector = operands[9:]
    row_count, width = tokens.shape
    groups = GROUPS
    rows = row_count // groups
    experts, _, hidden = gate.shape
    shared_cols = sgate.shape[1]
    quarter = width // ranks_tp
    chunks = CHUNKS
    chunk_width = quarter // chunks
    heads = query.shape[1] // HEAD_DIM
    length, lanes = cache.shape[1:]
    table_width = -(-2 * ranks_ep * experts // LANES) * LANES
    swaps = max(ranks_tp - 1, 1)
    all_rows = ranks_ep * rows
    half_rows = all_rows // 2
    away = max(ranks_ep // 2 - 1, 1)
    vmem = pl.BlockSpec(memory_space=pltpu.VMEM)
    hbm = pl.BlockSpec(memory_space=pltpu.HBM)
    dma = pltpu.SemaphoreType.DMA

    def store(*shape, dtype=BF16):
        return pltpu.VMEM(shape, dtype)

    def like(array):
        return pltpu.VMEM(array.shape, array.dtype)

    return pl.pallas_call(
        functools.partial(layer_kernel, ranks_ep, ranks_tp),
        out_shape=(
            jax.ShapeDtypeStruct((row_count, quarter), BF16),
            jax.ShapeDtypeStruct((row_count, 2 * key.shape[1]), BF16),
        ),
        in_specs=[hbm] * len(operands),
        out_specs=(vmem, vmem),
        scratch_shapes=[
            like(tokens),
            pltpu.SMEM(lengths.shape, lengths.dtype),
            like(cache),
            like(operands[3]),
            like(query),
            like(key),
            like(value),
            pltpu.SMEM(bias.shape, bias.dtype),
            like(out_weight),
            like(operands[9]),
            like(routes),
            like(portions),
            like(gate),
            like(up),
            like(down),
            like(sgate),
            like(sup),
            like(sdown),
            like(vector),
            store(row_count, width),
            store(rows * heads, length, dtype=F32),
            store(row_count, heads, lanes, dtype=F32),
            store(groups, rows, width),
            store(groups, swaps, rows, width),
            store(row_count, width, dtype=F32),
            store(groups, all_rows, width + table_width),
            store(groups, experts, all_rows, hidden),
            store(groups, chunks, ranks_tp, all_rows, chunk_width),
            store(groups, chunks, ranks_tp, half_rows, chunk_width),
            store(groups, chunks, ranks_tp, half_rows, chunk_width),
            store(groups, chunks, swaps, half_rows, chunk_width),
            store(groups, chunks, half_rows, chunk_width),
            store(groups, chunks, away, rows, chunk_width),
            store(groups, all_rows, 2 * shared_cols),
            store(groups, half_rows, 2 * shared_cols),
            store(groups, half_rows, 2 * shared_cols),
            store(groups, away, rows, 2 * shared_cols),
            store(groups, ranks_tp, rows, quarter),
            store(groups, swaps, rows, quarter),
            dma((24,)),
            dma((row_count,)),
            dma((groups, swaps)),
            dma((groups, swaps)),
            dma((groups, ranks_ep)),
            dma((groups, ranks_ep)),
            dma((groups, chunks)),
            dma((groups, chunks)),
            dma((groups, chunks, swaps)),
            dma((groups, chunks, swaps)),
            dma((groups, chunks, away)),
            dma((groups, chunks, away)),
            dma((groups,)),
            dma((groups,)),
            dma((groups, away)),
            dma((groups, away)),
            dma((groups, swaps)),
            dma((groups, swaps)),
        ],
        compiler_params=pltpu.CompilerParams(
            collective_id=0, has_side_effects=True, vmem_limit_bytes=60 * 2**20
        ),
    )(*operands)


def shards(
    ranks_ep,
    ranks_tp,
    tokens,
    lengths,
    cache,
    attn_gain,
    query_weight,
    key_weight,
    value_weight,
    stick_bias,
    out_weight,
    ffn_gain,
    routes,
    route_weights,
    expert_gate,
    expert_up,
    expert_down,
    shared_gate,
    shared_up,
    shared_down,
    gate_vector,
):
    width = tokens.shape[1]
    depth = shared_gate.shape[0]
    if depth % LANES:
        slot = lax.axis_index("ep") * depth % LANES
        wide = jnp.zeros((LANES, shared_gate.shape[1]), BF16)
        shared_gate = lax.dynamic_update_slice_in_dim(wide, shared_gate, slot, 0)
        shared_up = lax.dynamic_update_slice_in_dim(wide, shared_up, slot, 0)
    return layer(
        ranks_ep,
        ranks_tp,
        tokens,
        lengths,
        cache,
        attn_gain.reshape(1, width),
        query_weight,
        key_weight,
        value_weight,
        stick_bias,
        out_weight,
        ffn_gain.reshape(1, width),
        routes.T,
        route_weights.T,
        expert_gate,
        expert_up,
        expert_down,
        shared_gate,
        shared_up,
        shared_down,
        gate_vector,
    )


def solution(mesh):
    placed = (
        P("ep", None),
        P("ep"),
        P("ep", None, "tp"),
        P(),
        P(None, "tp"),
        P(None, "tp"),
        P(None, "tp"),
        P("tp"),
        P("tp", None),
        P(),
        P("ep", None),
        P("ep", None),
        P("ep", None, "tp"),
        P("ep", None, "tp"),
        P("ep", "tp", None),
        P("ep", "tp"),
        P("ep", "tp"),
        P("tp", None),
        P(),
    )
    return jax.shard_map(
        functools.partial(shards, mesh.shape["ep"], mesh.shape["tp"]),
        mesh=mesh,
        in_specs=placed,
        out_specs=(P("ep", "tp"), P("ep", "tp")),
        check_vma=False,
    )
```
